32 devices in a mesh: tp: 8 (over z, y), dp: 4 (over x, core).
Axes of the slice: x: 2, y: 2, z: 4, core: 2. Of those that a mesh axis runs over, the one named last changes fastest.
Arguments:
- tokens: bfloat16 [32, 4096], P('dp', 'tp'), may hold values from -6 to 6
- norm_gain: float32 [2, 4096], replicated, may hold values from 0.1 to 1.9
- w_query: bfloat16 [2, 4096, 2048], P(None, 'dp', 'tp'), may hold values from -0.09375 to 0.09375
- w_key: bfloat16 [2, 4096, 2048], P(None, 'dp', 'tp'), may hold values from -0.09375 to 0.09375
- w_value: bfloat16 [2, 4096, 4096], P(None, 'dp', 'tp'), may hold values from -0.09375 to 0.09375
- w_outgate: bfloat16 [2, 4096, 4096], P(None, 'dp', 'tp'), may hold values from -0.09375 to 0.09375
- w_ingate: bfloat16 [2, 4096, 16], P(None, 'dp'), may hold values from -0.09375 to 0.09375
- w_forget: bfloat16 [2, 4096, 16], P(None, 'dp'), may hold values from -0.09375 to 0.09375
- forget_bias: float32 [2, 16], replicated, may hold values from -2 to 5
- w_output: bfloat16 [2, 4096, 4096], P(None, 'dp', 'tp'), may hold values from -0.09375 to 0.09375
- mem_state: float32 [2, 32, 4096, 128], P(None, 'dp', 'tp'), may hold values from -0.8 to 0.8
- norm_state: float32 [2, 32, 16, 128], P(None, 'dp'), may hold values from -0.8 to 0.8
- max_state: float32 [2, 32, 16], P(None, 'dp'), may hold values from -4 to 4
Outputs:
- mixed: bfloat16 [32, 4096], P('dp', 'tp')
- new_memory: float32 [2, 32, 4096, 128], P(None, 'dp', 'tp')
- new_normaliser: float32 [2, 32, 16, 128], P(None, 'dp')
- new_stabiliser: float32 [2, 32, 16], P(None, 'dp')
The draws below stay inside these ranges and needn't reach their ends.
All inputs are finite; a program needn't handle non-finite values.
Results may differ from the reference program's by a relative error of at most 0.013.
Values may be sent and summed in bfloat16 or wider, within the bound.
A program may use at most 128 MiB of HBM per device.

```python
import jax
import jax.numpy as jnp
from jax import lax

D = 4096
H = 16
DK = 128
DV = 256
BLOCKS = 2
SEQS = 32


def levels(own_key, shape, split, least, top_value):
    def one(position, blocks):
        steps = jax.random.uniform(jax.random.fold_in(jax.random.fold_in(own_key, 6), position), (blocks,), jnp.float32, least / len(split), top_value / len(split))
        return jnp.repeat(jnp.exp(steps), shape[position] // blocks).reshape((-1,) + (1,) * (len(shape) - position - 1))

    level = one(*split[0])
    for cut in split[1:]:
        level = level * one(*cut)
    return level


def gaussian(own_key, dims, deviation, limit, cuts=(), dtype=jnp.bfloat16):
    entries = jax.random.normal(own_key, dims, jnp.float32) * deviation
    if len(cuts) > 0:
        entries = levels(own_key, dims, cuts, -0.22, 0.18) * entries
    return jnp.clip(entries, min=-limit, max=limit).astype(dtype)


def setup_inputs(seed: int = 0) -> dict:
    splits = jax.random.split(jax.random.key(seed), 14)
    return {
        "tokens": gaussian(splits[0], (SEQS, D), 1.0, 6.0, ((0, 4), (1, 8))),
        "norm_gain": jnp.clip(1.0 + 0.18 * jax.random.normal(splits[1], (BLOCKS, D), jnp.float32), 0.1, 1.9),
        "w_query": gaussian(splits[2], (BLOCKS, D, H * DK), D ** -0.5, 0.09375, ((1, 4), (2, 8))),
        "w_key": gaussian(splits[3], (BLOCKS, D, H * DK), D ** -0.5, 0.09375, ((1, 4), (2, 8))),
        "w_value": gaussian(splits[4], (BLOCKS, D, H * DV), D ** -0.5, 0.09375, ((1, 4), (2, 8))),
        "w_outgate": gaussian(splits[5], (BLOCKS, D, H * DV), D ** -0.5, 0.09375, ((1, 4), (2, 8))),
        "w_ingate": gaussian(splits[6], (BLOCKS, D, H), D ** -0.5, 0.09375, ((1, 4),)),
        "w_forget": gaussian(splits[7], (BLOCKS, D, H), D ** -0.5, 0.09375, ((1, 4),)),
        "forget_bias": jnp.clip(jax.random.uniform(splits[8], (BLOCKS, H), jnp.float32, -2.0, 5.0), -2.0, 5.0),
        "w_output": gaussian(splits[9], (BLOCKS, H * DV, D), (H * DV) ** -0.5, 0.09375, ((1, 4), (2, 8))),
        "mem_state": gaussian(splits[10], (BLOCKS, SEQS, H * DV, DK), 0.1, 0.8, ((1, 4), (2, 8)), jnp.float32),
        "norm_state": gaussian(splits[11], (BLOCKS, SEQS, H, DK), 0.1, 0.8, ((1, 4),), jnp.float32),
        "max_state": gaussian(splits[12], (BLOCKS, SEQS, H), 1.0, 4.0, ((1, 4),), jnp.float32),
    }


EPSILON = 1e-06

def mlstm_block(current, gain, w_query, w_key, w_value, w_outgate, w_ingate, w_forget, bias, w_output, memory, normaliser, stabiliser):
    seq_count = current.shape[0]
    wide = current.astype(jnp.float32)
    scale = lax.rsqrt(lax.optimization_barrier(jnp.mean(wide * wide, axis=-1, keepdims=True)) + EPSILON)
    normed = (wide * scale * gain).astype(jnp.bfloat16)
    query = jnp.dot(normed, w_query, preferred_element_type=jnp.float32).astype(jnp.bfloat16)
    keys = jnp.dot(normed, w_key, preferred_element_type=jnp.float32).astype(jnp.bfloat16)
    values = jnp.dot(normed, w_value, preferred_element_type=jnp.float32).astype(jnp.bfloat16)
    outgate = jnp.dot(normed, w_outgate, preferred_element_type=jnp.float32).astype(jnp.bfloat16)
    in_pre = jnp.dot(normed, w_ingate, preferred_element_type=jnp.float32)
    forget_pre = jnp.dot(normed, w_forget, preferred_element_type=jnp.float32)
    log_forget = jax.nn.log_sigmoid(forget_pre + bias)
    new_max = jnp.maximum(log_forget + stabiliser, in_pre)
    carried = jnp.exp(log_forget + stabiliser - new_max)
    fresh = jnp.exp(in_pre - new_max)
    query_heads = query.astype(jnp.float32).reshape(seq_count, H, DK)
    key_heads = keys.astype(jnp.float32).reshape(seq_count, H, DK) * DK ** (-0.5)
    value_heads = values.astype(jnp.float32).reshape(seq_count, H, DV)
    state = memory.reshape(seq_count, H, DV, DK)
    new_state = carried[:, :, None, None] * state + fresh[:, :, None, None] * value_heads[:, :, :, None] * key_heads[:, :, None, :]
    new_norm = carried[:, :, None] * normaliser + fresh[:, :, None] * key_heads
    divisor = jnp.maximum(jnp.abs(lax.optimization_barrier(jnp.sum(new_norm * query_heads, axis=-1))), 1.0)
    readout = lax.optimization_barrier(jnp.sum(new_state * query_heads[:, :, None, :], axis=-1)) / divisor[:, :, None]
    gated = (jax.nn.sigmoid(outgate.astype(jnp.float32)) * readout.reshape(seq_count, H * DV)).astype(jnp.bfloat16)
    update = jnp.dot(gated, w_output, preferred_element_type=jnp.float32)
    return ((wide + update).astype(jnp.bfloat16), new_state.reshape(seq_count, H * DV, DK), new_norm, new_max)

def reference(tokens, norm_gain, w_query, w_key, w_value, w_outgate, w_ingate, w_forget, forget_bias, w_output, mem_state, norm_state, max_state):
    current = tokens
    memories, normalisers, maxima = ([], [], [])
    for layer in range(BLOCKS):
        current, memory, normaliser, stabiliser = mlstm_block(current, norm_gain[layer], w_query[layer], w_key[layer], w_value[layer], w_outgate[layer], w_ingate[layer], w_forget[layer], forget_bias[layer], w_output[layer], mem_state[layer], norm_state[layer], max_state[layer])
        memories.append(memory)
        normalisers.append(normaliser)
        maxima.append(stabiliser)
    return (current, jnp.stack(memories), jnp.stack(normalisers), jnp.stack(maxima))
```

```python
import functools

import jax
import jax.numpy as jnp
from jax import lax
from jax.experimental import pallas as pl
from jax.experimental.pallas import tpu as pltpu
from jax.sharding import PartitionSpec as P

H = 16
DK = 128
DV = 256
BLOCKS = 2


EPSILON = 1e-06


def full_rows(shard):
    return lax.all_gather(shard, "tp", axis=1, tiled=True)


def fold_with(activations, pieces):
    return tuple(
        (jnp.dot(activations, piece, preferred_element_type=jnp.float32) for piece in pieces)
    )


def gathered(
    tokens,
    norm_gain,
    w_query,
    w_key,
    w_value,
    w_outgate,
    w_ingate,
    w_forget,
    forget_bias,
    w_output,
    mem_state,
    norm_state,
    max_state,
):
    seq_count = tokens.shape[0]
    value_cols = w_value.shape[2]
    column_head = (
        lax.axis_index("tp") * value_cols + jnp.arange(value_cols, dtype=jnp.int32)
    ) // DV
    current = tokens
    memories, normalisers, maxima = ([], [], [])
    for layer in range(BLOCKS):
        whole = full_rows(current)
        wide = whole.astype(jnp.float32)
        scale = lax.rsqrt(jnp.mean(wide * wide, axis=-1, keepdims=True) + EPSILON)
        normed = (wide * scale * norm_gain[layer]).astype(jnp.bfloat16)
        parts = fold_with(
            normed,
            (
                lax.all_gather(w_query[layer], "dp", axis=0, tiled=True),
                lax.all_gather(w_key[layer], "dp", axis=0, tiled=True),
                lax.all_gather(w_value[layer], "dp", axis=0, tiled=True),
                lax.all_gather(w_outgate[layer], "dp", axis=0, tiled=True),
                lax.all_gather(w_ingate[layer], "dp", axis=0, tiled=True),
                lax.all_gather(w_forget[layer], "dp", axis=0, tiled=True),
            ),
        )
        query = parts[0].astype(jnp.bfloat16)
        keys = parts[1].astype(jnp.bfloat16)
        values = parts[2].astype(jnp.bfloat16)
        outgate = parts[3].astype(jnp.bfloat16)
        in_pre = parts[4]
        forget_pre = parts[5]
        query_all, keys_all = (
            lax.all_gather(query, "tp", axis=1, tiled=True),
            lax.all_gather(keys, "tp", axis=1, tiled=True),
        )
        log_forget = jax.nn.log_sigmoid(forget_pre + forget_bias[layer])
        new_max = jnp.maximum(log_forget + max_state[layer], in_pre)
        carried = jnp.exp(log_forget + max_state[layer] - new_max)
        fresh = jnp.exp(in_pre - new_max)
        query_heads = query_all.astype(jnp.float32).reshape(seq_count, H, DK)
        key_heads = keys_all.astype(jnp.float32).reshape(seq_count, H, DK) * DK ** (-0.5)
        new_norm = carried[:, :, None] * norm_state[layer] + fresh[:, :, None] * key_heads
        divisor = jnp.maximum(jnp.abs(jnp.sum(new_norm * query_heads, axis=-1)), 1.0)
        query_cols = jnp.take(query_heads, column_head, axis=1)
        key_cols = jnp.take(key_heads, column_head, axis=1)
        carried_cols = jnp.take(carried, column_head, axis=1)
        fresh_cols = jnp.take(fresh, column_head, axis=1)
        divisor_cols = jnp.take(divisor, column_head, axis=1)
        value_wide = values.astype(jnp.float32)
        new_state = (
            carried_cols[:, :, None] * mem_state[layer]
            + fresh_cols[:, :, None] * value_wide[:, :, None] * key_cols
        )
        readout = jnp.sum(new_state * query_cols, axis=-1) / divisor_cols
        gated = (jax.nn.sigmoid(outgate.astype(jnp.float32)) * readout).astype(jnp.bfloat16)
        gated_rows = full_rows(gated)
        update = jnp.dot(
            gated_rows,
            lax.all_gather(w_output[layer], "dp", axis=0, tiled=True),
            preferred_element_type=jnp.float32,
        )
        current = (current.astype(jnp.float32) + update).astype(jnp.bfloat16)
        memories.append(new_state)
        normalisers.append(new_norm)
        maxima.append(new_max)
    return (current, jnp.stack(memories), jnp.stack(normalisers), jnp.stack(maxima))


WIRE = jnp.bfloat16
MESH = pl.DeviceIdType.MESH


def fused_kernel(
    tp, dp,
    tokens, gain, w_query, w_key, w_value, w_outgate, w_in, w_fg, bias, w_output, mem, norm, peak,
    mixed, mem_out, norm_out, peak_out,
    wq, wk, wv, wo, wi, wf, wp, state,
    cur, xg, gs, cg, part, got, gate_part, gate_got, up_part, up_got, nn,
    load_sem, out_sem, xs_sem, xr_sem, gs_sem, gr_sem, ps_sem, pr_sem, us_sem, ur_sem, ns_sem, nr_sem,
):
    t, d = lax.axis_index("tp"), lax.axis_index("dp")
    seqs, feats = tokens.shape
    rows = wq.shape[1]
    qcols, vcols = wq.shape[2], wv.shape[2]
    group = rows // feats
    own_heads = vcols // DV
    features = gain.shape[1]
    heads = peak.shape[2]
    f32, bf16 = jnp.float32, jnp.bfloat16

    loads = {}
    order = ((w_in, wi), (w_fg, wf), (w_query, wq), (w_key, wk), (w_value, wv), (w_outgate, wo), (mem, state), (w_output, wp))
    for b in range(BLOCKS):
        for i, (src, dst) in enumerate(order):
            c = pltpu.make_async_copy(src.at[b], dst.at[b], load_sem.at[b, i])
            c.start()
            loads[b, i] = c

    sends = []

    def spread(src, dst, send_sem, recv_sem):
        home, slot = t // group, t % group
        here = home == d

        def to(target, k):
            return pltpu.make_async_remote_copy(
                src_ref=src, dst_ref=dst.at[d, slot], send_sem=send_sem.at[k], recv_sem=recv_sem.at[d, slot],
                device_id={"tp": target, "dp": home}, device_id_type=MESH,
            )

        for k in range(tp - 1, 0, -1):
            c = to((t + k) % tp, k)
            c.start()
            sends.append((None, c))

        @pl.when(jnp.logical_not(here))
        def _():
            to(t, 0).start()

        @pl.when(here)
        def _():
            dst[d, slot] = src[...]

        sends.append((jnp.logical_not(here), to(t, 0)))

    def collect(dst, send_sem, recv_sem, dd, g):
        @pl.when(jnp.logical_or(d * group + g != t, d != dd))
        def _():
            pltpu.make_async_remote_copy(
                src_ref=dst.at[dd, g], dst_ref=dst.at[dd, g], send_sem=send_sem.at[0], recv_sem=recv_sem.at[dd, g],
                device_id={"tp": (t + 1) % tp, "dp": d}, device_id_type=MESH,
            ).wait_recv()

    def to_owners(src, dst, send_sem, recv_sem, view):
        copies = []
        for k in range(1, dp):
            dd = (d + k) % dp
            c = pltpu.make_async_remote_copy(
                src_ref=src.at[(dd,) + view], dst_ref=dst.at[(k - 1,) + view],
                send_sem=send_sem.at[k - 1], recv_sem=recv_sem.at[k - 1],
                device_id={"tp": t, "dp": dd}, device_id_type=MESH,
            )
            c.start()
            copies.append(c)
            sends.append((None, c))
        return copies

    def total(src, dst, view, copies):
        acc = src[(d,) + view].astype(f32)
        for k in range(dp - 1):
            copies[k].wait_recv()
            acc = acc + dst[(k,) + view].astype(f32)
        return acc

    gate_part[...] = jnp.zeros_like(gate_part)
    norms = []
    lane = lax.broadcasted_iota(jnp.int32, (seqs, heads), 1)
    row = lax.broadcasted_iota(jnp.int32, (seqs, DV), 0)
    everything = (slice(None), slice(None), slice(None))

    for b in range(BLOCKS):
        here = tokens if b == 0 else cur.at[b]
        spread(here, xg.at[b], xs_sem.at[b], xr_sem.at[b])
        for dd in range(dp):
            for g in range(group):
                collect(xg.at[b], xs_sem.at[b], xr_sem.at[b], dd, g)
        pieces = []
        square = jnp.zeros((dp * seqs, 1), f32)
        for g in range(group):
            wide = jnp.concatenate([xg[b, dd, g].astype(f32) for dd in range(dp)], axis=0)
            square = square + jnp.sum(wide * wide, axis=1, keepdims=True)
            at = pl.multiple_of(d * rows + g * feats, feats)
            pieces.append((wide * gain[b : b + 1, pl.ds(at, feats)]).astype(bf16))
        x = jnp.concatenate(pieces, axis=1)

        loads[b, 0].wait()
        loads[b, 1].wait()
        pre = (jnp.dot(x, wi[b], preferred_element_type=f32), jnp.dot(x, wf[b], preferred_element_type=f32))
        for dd in range(dp):
            own = slice(dd * seqs, (dd + 1) * seqs)
            gate_part[b, dd, 0, :, 0:heads] = pre[0][own]
            gate_part[b, dd, 1, :, 0:heads] = pre[1][own]
            gate_part[b, dd, 2] = jnp.broadcast_to(square[own], (seqs, gate_part.shape[-1]))
        gate_copies = to_owners(gate_part.at[b], gate_got.at[b], ps_sem.at[b, 0], pr_sem.at[b, 0], everything)

        spans, flights, at = [], [], 0
        for chunk, members in enumerate((((2, wq), (3, wk)), ((4, wv),), ((5, wo),))):
            begin = at
            for i, w in members:
                loads[b, i].wait()
                p = jnp.dot(x, w[b], preferred_element_type=f32).astype(WIRE)
                n = w.shape[2]
                for dd in range(dp):
                    part[b, dd, :, at : at + n] = p[dd * seqs : (dd + 1) * seqs]
                at += n
            view = (slice(None), pl.ds(begin, at - begin))
            spans.append(view)
            flights.append(to_owners(part.at[b], got.at[b], ps_sem.at[b, chunk + 1], pr_sem.at[b, chunk + 1], view))

        gates = total(gate_part.at[b], gate_got.at[b], everything, gate_copies)
        scale = lax.rsqrt(gates[2][:, 0:1] * (1.0 / features) + EPSILON)
        in_pre = gates[0][:, :heads] * scale
        forget = gates[1][:, :heads] * scale + bias[b : b + 1, :]
        log_forget = jnp.minimum(forget, 0.0) - jnp.log1p(jnp.exp(-jnp.abs(forget)))
        moved = log_forget + peak[b]
        new_peak = jnp.maximum(moved, in_pre)
        carried = jnp.exp(moved - new_peak)
        fresh = jnp.exp(in_pre - new_peak)
        peak_out[b] = new_peak

        qk = (total(part.at[b], got.at[b], spans[0], flights[0]) * scale).astype(bf16).astype(f32)
        loads[b, 6].wait()
        stage = []
        for hh in range(own_heads):
            mine = lane == t * own_heads + hh
            c_h = jnp.sum(jnp.where(mine, carried, 0.0), axis=1, keepdims=True)
            f_h = jnp.sum(jnp.where(mine, fresh, 0.0), axis=1, keepdims=True)
            q_h = qk[:, hh * DK : (hh + 1) * DK]
            k_h = qk[:, qcols + hh * DK : qcols + (hh + 1) * DK] * DK ** (-0.5)
            n_h = c_h * norm[b, :, t * own_heads + hh, :] + f_h * k_h
            nn[b, t, hh] = n_h
            div = jnp.maximum(jnp.abs(jnp.sum(n_h * q_h, axis=1, keepdims=True)), 1.0)
            kq = jnp.sum(k_h * q_h, axis=1, keepdims=True)
            q_b = q_h.astype(bf16)
            read = jnp.zeros((seqs, DV), f32)
            for s in range(seqs):
                c = state[b, s, hh * DV : (hh + 1) * DV, :].astype(bf16)
                r = lax.dot_general(q_b, c, (((1,), (1,)), ((), ())), preferred_element_type=f32)
                read = read + jnp.where(row == s, r, 0.0)
            stage.append((c_h, f_h, k_h, div, kq, read))

        v = (total(part.at[b], got.at[b], spans[1], flights[1]) * scale).astype(bf16).astype(f32)
        o = (total(part.at[b], got.at[b], spans[2], flights[2]) * scale).astype(bf16).astype(f32)
        for hh, (c_h, f_h, k_h, div, kq, read) in enumerate(stage):
            cols = slice(hh * DV, (hh + 1) * DV)
            readout = (c_h * read + (f_h * kq) * v[:, cols]) / div
            gs[b, :, cols] = (jax.nn.sigmoid(o[:, cols]) * readout).astype(bf16)
        spread(gs.at[b], cg.at[b], gs_sem.at[b], gr_sem.at[b])

        for k in range(1, tp):
            c = pltpu.make_async_remote_copy(
                src_ref=nn.at[b, t], dst_ref=nn.at[b, t], send_sem=ns_sem.at[b, k - 1], recv_sem=nr_sem.at[b, k - 1],
                device_id={"tp": (t + k) % tp, "dp": d}, device_id_type=MESH,
            )
            c.start()
            sends.append((None, c))
            norms.append((k, b))

        for hh, (c_h, f_h, k_h, div, kq, read) in enumerate(stage):
            cols = slice(hh * DV, (hh + 1) * DV)
            v_t = jnp.transpose(v[:, cols] * f_h)
            for s in range(seqs):
                state[b, s, cols, :] = c_h[s : s + 1] * state[b, s, cols, :] + v_t[:, s : s + 1] * k_h[s : s + 1]
        store = pltpu.make_async_copy(state.at[b], mem_out.at[b], out_sem.at[b])
        store.start()
        loads[b, "store"] = store

        for dd in range(dp):
            for g in range(group):
                collect(cg.at[b], gs_sem.at[b], gr_sem.at[b], dd, g)
        gated = jnp.concatenate(
            [
                jnp.concatenate([cg[b, dd, g].astype(f32) for dd in range(dp)], axis=0).astype(bf16)
                for g in range(group)
            ],
            axis=1,
        )
        loads[b, 7].wait()
        up = jnp.dot(gated, wp[b], preferred_element_type=f32)
        for dd in range(dp):
            up_part[b, dd] = up[dd * seqs : (dd + 1) * seqs]
        flat = (slice(None), slice(None))
        copies = to_owners(up_part.at[b], up_got.at[b], us_sem.at[b], ur_sem.at[b], flat)
        update = total(up_part.at[b], up_got.at[b], flat, copies)
        after = (here[...].astype(f32) + update).astype(bf16)
        if b + 1 < BLOCKS:
            cur[b + 1] = after
        else:
            mixed[...] = after

    for k, b in norms:
        pltpu.make_async_remote_copy(
            src_ref=nn.at[b, t], dst_ref=nn.at[b, (t + tp - k) % tp], send_sem=ns_sem.at[b, k - 1],
            recv_sem=nr_sem.at[b, k - 1], device_id={"tp": (t + k) % tp, "dp": d}, device_id_type=MESH,
        ).wait_recv()
    for b in range(BLOCKS):
        for i in range(tp):
            for hh in range(own_heads):
                norm_out[b, i * own_heads + hh] = nn[b, i, hh]
        loads[b, "store"].wait()
    for cond, c in sends:
        if cond is None:
            c.wait_send()
        else:
            pl.when(cond)(c.wait_send)


def fused(tp, dp, tokens, gain, w_query, w_key, w_value, w_outgate, w_in, w_fg, bias, w_output, mem, norm, peak):
    seqs, feats = tokens.shape
    rows, vcols = w_value.shape[1:]
    group, own_heads = rows // feats, vcols // DV
    heads = peak.shape[2]
    width = 2 * w_query.shape[2] + 2 * vcols
    anywhere, vmem = pl.BlockSpec(memory_space=pl.ANY), pl.BlockSpec(memory_space=pltpu.VMEM)
    f32, bf16 = jnp.float32, jnp.bfloat16
    dma = pltpu.SemaphoreType.DMA
    big = (w_query, w_key, w_value, w_outgate, w_in, w_fg, w_output, mem)
    others = max(dp - 1, 1)
    mixed, new_mem, new_norm, new_peak = pl.pallas_call(
        functools.partial(fused_kernel, tp, dp),
        out_shape=(
            jax.ShapeDtypeStruct(tokens.shape, tokens.dtype),
            jax.ShapeDtypeStruct(mem.shape, mem.dtype),
            jax.ShapeDtypeStruct((BLOCKS, heads, seqs, DK), f32),
            jax.ShapeDtypeStruct(peak.shape, f32),
        ),
        in_specs=[vmem, vmem] + [anywhere] * 6 + [vmem, anywhere, anywhere, vmem, vmem],
        out_specs=(vmem, anywhere, vmem, vmem),
        scratch_shapes=[pltpu.VMEM(w.shape, w.dtype) for w in big]
        + [
            pltpu.VMEM((BLOCKS, seqs, feats), bf16),
            pltpu.VMEM((BLOCKS, dp, group, seqs, feats), bf16),
            pltpu.VMEM((BLOCKS, seqs, vcols), bf16),
            pltpu.VMEM((BLOCKS, dp, group, seqs, vcols), bf16),
            pltpu.VMEM((BLOCKS, dp, seqs, width), WIRE),
            pltpu.VMEM((BLOCKS, others, seqs, width), WIRE),
            pltpu.VMEM((BLOCKS, dp, 3, seqs, 128), f32),
            pltpu.VMEM((BLOCKS, others, 3, seqs, 128), f32),
            pltpu.VMEM((BLOCKS, dp, seqs, feats), f32),
            pltpu.VMEM((BLOCKS, others, seqs, feats), f32),
            pltpu.VMEM((BLOCKS, tp, own_heads, seqs, DK), f32),
            dma((BLOCKS, 8)),
            dma((BLOCKS,)),
            dma((BLOCKS, tp)),
            dma((BLOCKS, dp, group)),
            dma((BLOCKS, tp)),
            dma((BLOCKS, dp, group)),
            dma((BLOCKS, 4, others)),
            dma((BLOCKS, 4, others)),
            dma((BLOCKS, others)),
            dma((BLOCKS, others)),
            dma((BLOCKS, tp)),
            dma((BLOCKS, tp)),
        ],
        compiler_params=pltpu.CompilerParams(has_side_effects=True, vmem_limit_bytes=60 * 1024 * 1024),
    )(tokens, gain, w_query, w_key, w_value, w_outgate, w_in, w_fg, bias, w_output, mem, norm, peak)
    return mixed, new_mem, jnp.transpose(new_norm, (0, 2, 1, 3)), new_peak


def whole_heads(tp, dp, *args):
    tokens, w_query, w_value, w_output = args[0], args[2], args[4], args[9]
    seqs, feats = tokens.shape
    rows, vcols = w_value.shape[1:]
    return (
        tp > 1 and dp > 1 and seqs % 8 == 0 and feats % 128 == 0
        and vcols % DV == 0 and w_query.shape[2] == vcols // DV * DK
        and rows % feats == 0 and vcols == feats and w_output.shape[1] == rows
    )


def shards(tp, dp, *args):
    if whole_heads(tp, dp, *args):
        return fused(tp, dp, *args)
    return gathered(*args)


def solution(mesh):
    in_specs = (
        P("dp", "tp"),
        P(),
        P(None, "dp", "tp"),
        P(None, "dp", "tp"),
        P(None, "dp", "tp"),
        P(None, "dp", "tp"),
        P(None, "dp", None),
        P(None, "dp", None),
        P(),
        P(None, "dp", "tp"),
        P(None, "dp", "tp", None),
        P(None, "dp", None, None),
        P(None, "dp", None),
    )
    out_specs = (
        P("dp", "tp"),
        P(None, "dp", "tp", None),
        P(None, "dp", None, None),
        P(None, "dp", None),
    )
    body = functools.partial(shards, mesh.shape["tp"], mesh.shape["dp"])
    return jax.shard_map(body, mesh=mesh, in_specs=in_specs, out_specs=out_specs, check_vma=False)
```

```python
import functools

import jax
import jax.numpy as jnp
from jax import lax
from jax.experimental import pallas as pl
from jax.experimental.pallas import tpu as pltpu
from jax.sharding import PartitionSpec as P

H = 16
DK = 128
DV = 256
BLOCKS = 2


EPSILON = 1e-06


def full_rows(shard):
    return lax.all_gather(shard, "tp", axis=1, tiled=True)


def fold_with(activations, pieces):
    return tuple(
        (jnp.dot(activations, piece, preferred_element_type=jnp.float32) for piece in pieces)
    )


def gathered(
    tokens,
    norm_gain,
    w_query,
    w_key,
    w_value,
    w_outgate,
    w_ingate,
    w_forget,
    forget_bias,
    w_output,
    mem_state,
    norm_state,
    max_state,
):
    seq_count = tokens.shape[0]
    value_cols = w_value.shape[2]
    column_head = (
        lax.axis_index("tp") * value_cols + jnp.arange(value_cols, dtype=jnp.int32)
    ) // DV
    current = tokens
    memories, normalisers, maxima = ([], [], [])
    for layer in range(BLOCKS):
        whole = full_rows(current)
        wide = whole.astype(jnp.float32)
        scale = lax.rsqrt(jnp.mean(wide * wide, axis=-1, keepdims=True) + EPSILON)
        normed = (wide * scale * norm_gain[layer]).astype(jnp.bfloat16)
        parts = fold_with(
            normed,
            (
                lax.all_gather(w_query[layer], "dp", axis=0, tiled=True),
                lax.all_gather(w_key[layer], "dp", axis=0, tiled=True),
                lax.all_gather(w_value[layer], "dp", axis=0, tiled=True),
                lax.all_gather(w_outgate[layer], "dp", axis=0, tiled=True),
                lax.all_gather(w_ingate[layer], "dp", axis=0, tiled=True),
                lax.all_gather(w_forget[layer], "dp", axis=0, tiled=True),
            ),
        )
        query = parts[0].astype(jnp.bfloat16)
        keys = parts[1].astype(jnp.bfloat16)
        values = parts[2].astype(jnp.bfloat16)
        outgate = parts[3].astype(jnp.bfloat16)
        in_pre = parts[4]
        forget_pre = parts[5]
        query_all, keys_all = (
            lax.all_gather(query, "tp", axis=1, tiled=True),
            lax.all_gather(keys, "tp", axis=1, tiled=True),
        )
        log_forget = jax.nn.log_sigmoid(forget_pre + forget_bias[layer])
        new_max = jnp.maximum(log_forget + max_state[layer], in_pre)
        carried = jnp.exp(log_forget + max_state[layer] - new_max)
        fresh = jnp.exp(in_pre - new_max)
        query_heads = query_all.astype(jnp.float32).reshape(seq_count, H, DK)
        key_heads = keys_all.astype(jnp.float32).reshape(seq_count, H, DK) * DK ** (-0.5)
        new_norm = carried[:, :, None] * norm_state[layer] + fresh[:, :, None] * key_heads
        divisor = jnp.maximum(jnp.abs(jnp.sum(new_norm * query_heads, axis=-1)), 1.0)
        query_cols = jnp.take(query_heads, column_head, axis=1)
        key_cols = jnp.take(key_heads, column_head, axis=1)
        carried_cols = jnp.take(carried, column_head, axis=1)
        fresh_cols = jnp.take(fresh, column_head, axis=1)
        divisor_cols = jnp.take(divisor, column_head, axis=1)
        value_wide = values.astype(jnp.float32)
        new_state = (
            carried_cols[:, :, None] * mem_state[layer]
            + fresh_cols[:, :, None] * value_wide[:, :, None] * key_cols
        )
        readout = jnp.sum(new_state * query_cols, axis=-1) / divisor_cols
        gated = (jax.nn.sigmoid(outgate.astype(jnp.float32)) * readout).astype(jnp.bfloat16)
        gated_rows = full_rows(gated)
        update = jnp.dot(
            gated_rows,
            lax.all_gather(w_output[layer], "dp", axis=0, tiled=True),
            preferred_element_type=jnp.float32,
        )
        current = (current.astype(jnp.float32) + update).astype(jnp.bfloat16)
        memories.append(new_state)
        normalisers.append(new_norm)
        maxima.append(new_max)
    return (current, jnp.stack(memories), jnp.stack(normalisers), jnp.stack(maxima))


WIRE = jnp.bfloat16
MESH = pl.DeviceIdType.MESH


def fused_kernel(
    tp, dp,
    tokens, gain_in, w_query, w_key, w_value, w_outgate, w_in, w_fg, bias_in, w_output, mem, norm_in, peak_in,
    mixed, state, norm_out, peak_out,
    wq, wk, wv, wo, wi, wp, gain, bias, norm, peak,
    cur, xg, gs, cg, part, got, gate_part, gate_got, up_part, up_got, nn,
    small_sem, load_sem, xs_sem, xr_sem, gs_sem, gr_sem, ps_sem, pr_sem, us_sem, ur_sem, ns_sem, nr_sem,
):
    t, d = lax.axis_index("tp"), lax.axis_index("dp")
    seqs, feats = tokens.shape
    rows = wq.shape[1]
    qcols, vcols = wq.shape[2], wv.shape[2]
    group = rows // feats
    own_heads = vcols // DV
    features = gain.shape[1]
    heads = peak.shape[2]
    f32, bf16 = jnp.float32, jnp.bfloat16

    smalls = []
    for i, (src, dst) in enumerate(
        ((tokens, cur.at[0]), (gain_in, gain), (bias_in, bias), (norm_in, norm), (peak_in, peak))
    ):
        c = pltpu.make_async_copy(src, dst, small_sem.at[i])
        c.start()
        smalls.append(c)
    loads = {}
    order = ((w_in, wi), (w_fg, wi), (w_query, wq), (w_key, wk), (w_value, wv), (w_outgate, wo), (mem, state), (w_output, wp))
    for b in range(BLOCKS):
        for i, (src, dst) in enumerate(order):
            to = dst.at[b, pl.ds(i * heads, heads)] if i < 2 else dst.at[b]
            c = pltpu.make_async_copy(src.at[b], to, load_sem.at[b, i])
            c.start()
            loads[b, i] = c

    barrier = pltpu.get_barrier_semaphore()
    for i in range(tp):
        for j in range(dp):
            if i + j > 0:
                there = {"tp": (t + i) % tp, "dp": (d + j) % dp}
                pl.semaphore_signal(barrier, inc=1, device_id=there, device_id_type=MESH)
    gate_part[...] = jnp.zeros_like(gate_part)
    for c in smalls:
        c.wait()
    pl.semaphore_wait(barrier, tp * dp - 1)

    sends = []

    def spread(src, dst, send_sem, recv_sem):
        home, slot = t // group, t % group
        here = home == d

        def to(target, k):
            return pltpu.make_async_remote_copy(
                src_ref=src, dst_ref=dst.at[d, slot], send_sem=send_sem.at[k], recv_sem=recv_sem.at[d, slot],
                device_id={"tp": target, "dp": home}, device_id_type=MESH,
            )

        for k in range(tp - 1, 0, -1):
            c = to((t + k) % tp, k)
            c.start()
            sends.append((None, c))

        @pl.when(jnp.logical_not(here))
        def _():
            to(t, 0).start()

        @pl.when(here)
        def _():
            dst[d, slot] = src[...]

        sends.append((jnp.logical_not(here), to(t, 0)))

    def collect(dst, send_sem, recv_sem, dd, g):
        @pl.when(jnp.logical_or(d * group + g != t, d != dd))
        def _():
            pltpu.make_async_remote_copy(
                src_ref=dst.at[dd, g], dst_ref=dst.at[dd, g], send_sem=send_sem.at[0], recv_sem=recv_sem.at[dd, g],
                device_id={"tp": (t + 1) % tp, "dp": d}, device_id_type=MESH,
            ).wait_recv()

    def to_owners(src, dst, send_sem, recv_sem, view):
        copies = []
        for k in range(1, dp):
            dd = (d + k) % dp
            c = pltpu.make_async_remote_copy(
                src_ref=src.at[(dd,) + view], dst_ref=dst.at[(k - 1,) + view],
                send_sem=send_sem.at[k - 1], recv_sem=recv_sem.at[k - 1],
                device_id={"tp": t, "dp": dd}, device_id_type=MESH,
            )
            c.start()
            copies.append(c)
            sends.append((None, c))
        return copies

    def total(src, dst, view, copies):
        acc = src[(d,) + view].astype(f32)
        for k in range(dp - 1):
            copies[k].wait_recv()
            acc = acc + dst[(k,) + view].astype(f32)
        return acc

    norms = []
    lane = lax.broadcasted_iota(jnp.int32, (seqs, heads), 1)
    row = lax.broadcasted_iota(jnp.int32, (seqs, DV), 0)
    everything = (slice(None), slice(None))

    for b in range(BLOCKS):
        here = cur.at[b]
        spread(here, xg.at[b], xs_sem.at[b], xr_sem.at[b])
        for dd in range(dp):
            for g in range(group):
                collect(xg.at[b], xs_sem.at[b], xr_sem.at[b], dd, g)
        pieces = []
        square = jnp.zeros((dp * seqs, 1), f32)
        for g in range(group):
            wide = jnp.concatenate([xg[b, dd, g].astype(f32) for dd in range(dp)], axis=0)
            square = square + jnp.sum(wide * wide, axis=1, keepdims=True)
            at = pl.multiple_of(d * rows + g * feats, feats)
            pieces.append((wide * gain[b : b + 1, pl.ds(at, feats)]).astype(bf16))
        x = jnp.concatenate(pieces, axis=1)

        loads[b, 0].wait()
        loads[b, 1].wait()
        pre = lax.dot_general(x, wi[b], (((1,), (1,)), ((), ())), preferred_element_type=f32)
        for dd in range(dp):
            own = slice(dd * seqs, (dd + 1) * seqs)
            gate_part[b, dd, :, 0 : 2 * heads] = pre[own]
            gate_part[b, dd, :, 2 * heads : 2 * heads + 1] = square[own]
        gate_copies = to_owners(gate_part.at[b], gate_got.at[b], ps_sem.at[b, 0], pr_sem.at[b, 0], everything)

        spans, flights, at = [], [], 0
        for chunk, members in enumerate((((2, wq), (3, wk)), ((4, wv),), ((5, wo),))):
            begin = at
            for i, w in members:
                loads[b, i].wait()
                p = jnp.dot(x, w[b], preferred_element_type=f32).astype(WIRE)
                n = w.shape[2]
                for dd in range(dp):
                    part[b, dd, :, at : at + n] = p[dd * seqs : (dd + 1) * seqs]
                at += n
            view = (slice(None), pl.ds(begin, at - begin))
            spans.append(view)
            flights.append(to_owners(part.at[b], got.at[b], ps_sem.at[b, chunk + 1], pr_sem.at[b, chunk + 1], view))

        gates = total(gate_part.at[b], gate_got.at[b], everything, gate_copies)
        scale = lax.rsqrt(gates[:, 2 * heads : 2 * heads + 1] * (1.0 / features) + EPSILON)
        in_pre = gates[:, :heads] * scale
        forget = gates[:, heads : 2 * heads] * scale + bias[b : b + 1, :]
        log_forget = jnp.minimum(forget, 0.0) - jnp.log1p(jnp.exp(-jnp.abs(forget)))
        moved = log_forget + peak[b]
        new_peak = jnp.maximum(moved, in_pre)
        carried = jnp.exp(moved - new_peak)
        fresh = jnp.exp(in_pre - new_peak)
        peak_out[b] = new_peak

        qk = (total(part.at[b], got.at[b], spans[0], flights[0]) * scale).astype(bf16).astype(f32)
        loads[b, 6].wait()
        stage = []
        for hh in range(own_heads):
            mine = lane == t * own_heads + hh
            c_h = jnp.sum(jnp.where(mine, carried, 0.0), axis=1, keepdims=True)
            f_h = jnp.sum(jnp.where(mine, fresh, 0.0), axis=1, keepdims=True)
            q_h = qk[:, hh * DK : (hh + 1) * DK]
            k_h = qk[:, qcols + hh * DK : qcols + (hh + 1) * DK] * DK ** (-0.5)
            n_h = c_h * norm[b, :, t * own_heads + hh, :] + f_h * k_h
            nn[b, t, hh] = n_h
            div = jnp.maximum(jnp.abs(jnp.sum(n_h * q_h, axis=1, keepdims=True)), 1.0)
            kq = jnp.sum(k_h * q_h, axis=1, keepdims=True)
            q_b = q_h.astype(bf16)
            read = jnp.zeros((seqs, DV), f32)
            for s in range(seqs):
                c = state[b, s, hh * DV : (hh + 1) * DV, :].astype(bf16)
                r = lax.dot_general(q_b, c, (((1,), (1,)), ((), ())), preferred_element_type=f32)
                read = read + jnp.where(row == s, r, 0.0)
            stage.append((c_h, f_h, k_h, div, kq, read))

        v = (total(part.at[b], got.at[b], spans[1], flights[1]) * scale).astype(bf16).astype(f32)
        o = (total(part.at[b], got.at[b], spans[2], flights[2]) * scale).astype(bf16).astype(f32)
        for hh, (c_h, f_h, k_h, div, kq, read) in enumerate(stage):
            cols = slice(hh * DV, (hh + 1) * DV)
            readout = (c_h * read + (f_h * kq) * v[:, cols]) / div
            gs[b, :, cols] = (jax.nn.sigmoid(o[:, cols]) * readout).astype(bf16)
        spread(gs.at[b], cg.at[b], gs_sem.at[b], gr_sem.at[b])

        for k in range(1, tp):
            c = pltpu.make_async_remote_copy(
                src_ref=nn.at[b, t], dst_ref=nn.at[b, t], send_sem=ns_sem.at[b, k - 1], recv_sem=nr_sem.at[b, k - 1],
                device_id={"tp": (t + k) % tp, "dp": d}, device_id_type=MESH,
            )
            c.start()
            sends.append((None, c))
            norms.append((k, b))

        for hh, (c_h, f_h, k_h, div, kq, read) in enumerate(stage):
            cols = slice(hh * DV, (hh + 1) * DV)
            v_t = jnp.transpose(v[:, cols] * f_h)
            for s in range(seqs):
                state[b, s, cols, :] = c_h[s : s + 1] * state[b, s, cols, :] + v_t[:, s : s + 1] * k_h[s : s + 1]
        for dd in range(dp):
            for g in range(group):
                collect(cg.at[b], gs_sem.at[b], gr_sem.at[b], dd, g)
        gated = jnp.concatenate(
            [
                jnp.concatenate([cg[b, dd, g].astype(f32) for dd in range(dp)], axis=0).astype(bf16)
                for g in range(group)
            ],
            axis=1,
        )
        loads[b, 7].wait()
        up = jnp.dot(gated, wp[b], preferred_element_type=f32)
        for dd in range(dp):
            up_part[b, dd] = up[dd * seqs : (dd + 1) * seqs]
        flat = (slice(None), slice(None))
        copies = to_owners(up_part.at[b], up_got.at[b], us_sem.at[b], ur_sem.at[b], flat)
        update = total(up_part.at[b], up_got.at[b], flat, copies)
        after = (here[...].astype(f32) + update).astype(bf16)
        if b + 1 < BLOCKS:
            cur[b + 1] = after
        else:
            mixed[...] = after

    for k, b in norms:
        pltpu.make_async_remote_copy(
            src_ref=nn.at[b, t], dst_ref=nn.at[b, (t + tp - k) % tp], send_sem=ns_sem.at[b, k - 1],
            recv_sem=nr_sem.at[b, k - 1], device_id={"tp": (t + k) % tp, "dp": d}, device_id_type=MESH,
        ).wait_recv()
    for b in range(BLOCKS):
        for i in range(tp):
            for hh in range(own_heads):
                norm_out[b, :, i * own_heads + hh, :] = nn[b, i, hh]
    for cond, c in sends:
        if cond is None:
            c.wait_send()
        else:
            pl.when(cond)(c.wait_send)


def write_kernel(*refs):
    count = (len(refs) - 1) // 2
    sem = refs[-1]
    copies = [pltpu.make_async_copy(refs[i], refs[count + i], sem.at[i]) for i in range(count)]
    for c in copies:
        c.start()
    for c in copies:
        c.wait()


def written(*arrays):
    return pl.pallas_call(
        write_kernel,
        out_shape=tuple(jax.ShapeDtypeStruct(a.shape, a.dtype) for a in arrays),
        in_specs=[pl.BlockSpec(memory_space=pltpu.VMEM)] * len(arrays),
        out_specs=(pl.BlockSpec(memory_space=pl.ANY),) * len(arrays),
        scratch_shapes=[pltpu.SemaphoreType.DMA((len(arrays),))],
        compiler_params=pltpu.CompilerParams(vmem_limit_bytes=1024 * 1024),
    )(*(pltpu.with_memory_space_constraint(a, pltpu.VMEM) for a in arrays))


def fused(tp, dp, tokens, gain, w_query, w_key, w_value, w_outgate, w_in, w_fg, bias, w_output, mem, norm, peak):
    seqs, feats = tokens.shape
    rows, vcols = w_value.shape[1:]
    group, own_heads = rows // feats, vcols // DV
    heads = peak.shape[2]
    width = 2 * w_query.shape[2] + 2 * vcols
    vmem = pl.BlockSpec(memory_space=pltpu.VMEM)
    f32, bf16 = jnp.float32, jnp.bfloat16
    dma = pltpu.SemaphoreType.DMA
    w_in, w_fg = jnp.swapaxes(w_in, 1, 2), jnp.swapaxes(w_fg, 1, 2)
    arrays = (tokens, gain, w_query, w_key, w_value, w_outgate, w_in, w_fg, bias, w_output, mem, norm, peak)
    gates = (BLOCKS, 2 * heads, rows)
    big = (w_query.shape, w_key.shape, w_value.shape, w_outgate.shape, gates, w_output.shape)
    lanes = -(-(2 * heads + 1) // 128) * 128
    others = max(dp - 1, 1)
    results = pl.pallas_call(
        functools.partial(fused_kernel, tp, dp),
        out_shape=(
            pltpu.VMEM(tokens.shape, tokens.dtype),
            pltpu.VMEM(mem.shape, mem.dtype),
            pltpu.VMEM(norm.shape, f32),
            pltpu.VMEM(peak.shape, f32),
        ),
        in_specs=[pl.BlockSpec(memory_space=pltpu.HBM)] * len(arrays),
        out_specs=(vmem, vmem, vmem, vmem),
        scratch_shapes=[pltpu.VMEM(shape, bf16) for shape in big]
        + [pltpu.VMEM(a.shape, a.dtype) for a in (gain, bias, norm, peak)]
        + [
            pltpu.VMEM((BLOCKS, seqs, feats), bf16),
            pltpu.VMEM((BLOCKS, dp, group, seqs, feats), bf16),
            pltpu.VMEM((BLOCKS, seqs, vcols), bf16),
            pltpu.VMEM((BLOCKS, dp, group, seqs, vcols), bf16),
            pltpu.VMEM((BLOCKS, dp, seqs, width), WIRE),
            pltpu.VMEM((BLOCKS, others, seqs, width), WIRE),
            pltpu.VMEM((BLOCKS, dp, seqs, lanes), f32),
            pltpu.VMEM((BLOCKS, others, seqs, lanes), f32),
            pltpu.VMEM((BLOCKS, dp, seqs, feats), f32),
            pltpu.VMEM((BLOCKS, others, seqs, feats), f32),
            pltpu.VMEM((BLOCKS, tp, own_heads, seqs, DK), f32),
            dma((5,)),
            dma((BLOCKS, 8)),
            dma((BLOCKS, tp)),
            dma((BLOCKS, dp, group)),
            dma((BLOCKS, tp)),
            dma((BLOCKS, dp, group)),
            dma((BLOCKS, 4, others)),
            dma((BLOCKS, 4, others)),
            dma((BLOCKS, others)),
            dma((BLOCKS, others)),
            dma((BLOCKS, tp)),
            dma((BLOCKS, tp)),
        ],
        compiler_params=pltpu.CompilerParams(
            collective_id=0, has_side_effects=True, vmem_limit_bytes=24 * 1024 * 1024
        ),
    )(*(pltpu.with_memory_space_constraint(a, pltpu.HBM) for a in arrays))
    return written(*results)


def whole_heads(tp, dp, *args):
    tokens, w_query, w_value, w_output = args[0], args[2], args[4], args[9]
    seqs, feats = tokens.shape
    rows, vcols = w_value.shape[1:]
    return (
        tp > 1 and dp > 1 and seqs % 8 == 0 and feats % 128 == 0
        and vcols % DV == 0 and w_query.shape[2] == vcols // DV * DK
        and rows % feats == 0 and vcols == feats and w_output.shape[1] == rows
    )


def shards(tp, dp, *args):
    if whole_heads(tp, dp, *args):
        return fused(tp, dp, *args)
    return gathered(*args)


def solution(mesh):
    in_specs = (
        P("dp", "tp"),
        P(),
        P(None, "dp", "tp"),
        P(None, "dp", "tp"),
        P(None, "dp", "tp"),
        P(None, "dp", "tp"),
        P(None, "dp", None),
        P(None, "dp", None),
        P(),
        P(None, "dp", "tp"),
        P(None, "dp", "tp", None),
        P(None, "dp", None, None),
        P(None, "dp", None),
    )
    out_specs = (
        P("dp", "tp"),
        P(None, "dp", "tp", None),
        P(None, "dp", None, None),
        P(None, "dp", None),
    )
    body = functools.partial(shards, mesh.shape["tp"], mesh.shape["dp"])
    return jax.shard_map(body, mesh=mesh, in_specs=in_specs, out_specs=out_specs, check_vma=False)
```

```python
import functools

import jax
import jax.numpy as jnp
from jax import lax
from jax.experimental import pallas as pl
from jax.experimental.pallas import tpu as pltpu
from jax.sharding import PartitionSpec as P

H = 16
DK = 128
DV = 256
BLOCKS = 2


EPSILON = 1e-06


def full_rows(shard):
    return lax.all_gather(shard, "tp", axis=1, tiled=True)


def fold_with(activations, pieces):
    return tuple(
        (jnp.dot(activations, piece, preferred_element_type=jnp.float32) for piece in pieces)
    )


def gathered(
    tokens,
    norm_gain,
    w_query,
    w_key,
    w_value,
    w_outgate,
    w_ingate,
    w_forget,
    forget_bias,
    w_output,
    mem_state,
    norm_state,
    max_state,
):
    seq_count = tokens.shape[0]
    value_cols = w_value.shape[2]
    column_head = (
        lax.axis_index("tp") * value_cols + jnp.arange(value_cols, dtype=jnp.int32)
    ) // DV
    current = tokens
    memories, normalisers, maxima = ([], [], [])
    for layer in range(BLOCKS):
        whole = full_rows(current)
        wide = whole.astype(jnp.float32)
        scale = lax.rsqrt(jnp.mean(wide * wide, axis=-1, keepdims=True) + EPSILON)
        normed = (wide * scale * norm_gain[layer]).astype(jnp.bfloat16)
        parts = fold_with(
            normed,
            (
                lax.all_gather(w_query[layer], "dp", axis=0, tiled=True),
                lax.all_gather(w_key[layer], "dp", axis=0, tiled=True),
                lax.all_gather(w_value[layer], "dp", axis=0, tiled=True),
                lax.all_gather(w_outgate[layer], "dp", axis=0, tiled=True),
                lax.all_gather(w_ingate[layer], "dp", axis=0, tiled=True),
                lax.all_gather(w_forget[layer], "dp", axis=0, tiled=True),
            ),
        )
        query = parts[0].astype(jnp.bfloat16)
        keys = parts[1].astype(jnp.bfloat16)
        values = parts[2].astype(jnp.bfloat16)
        outgate = parts[3].astype(jnp.bfloat16)
        in_pre = parts[4]
        forget_pre = parts[5]
        query_all, keys_all = (
            lax.all_gather(query, "tp", axis=1, tiled=True),
            lax.all_gather(keys, "tp", axis=1, tiled=True),
        )
        log_forget = jax.nn.log_sigmoid(forget_pre + forget_bias[layer])
        new_max = jnp.maximum(log_forget + max_state[layer], in_pre)
        carried = jnp.exp(log_forget + max_state[layer] - new_max)
        fresh = jnp.exp(in_pre - new_max)
        query_heads = query_all.astype(jnp.float32).reshape(seq_count, H, DK)
        key_heads = keys_all.astype(jnp.float32).reshape(seq_count, H, DK) * DK ** (-0.5)
        new_norm = carried[:, :, None] * norm_state[layer] + fresh[:, :, None] * key_heads
        divisor = jnp.maximum(jnp.abs(jnp.sum(new_norm * query_heads, axis=-1)), 1.0)
        query_cols = jnp.take(query_heads, column_head, axis=1)
        key_cols = jnp.take(key_heads, column_head, axis=1)
        carried_cols = jnp.take(carried, column_head, axis=1)
        fresh_cols = jnp.take(fresh, column_head, axis=1)
        divisor_cols = jnp.take(divisor, column_head, axis=1)
        value_wide = values.astype(jnp.float32)
        new_state = (
            carried_cols[:, :, None] * mem_state[layer]
            + fresh_cols[:, :, None] * value_wide[:, :, None] * key_cols
        )
        readout = jnp.sum(new_state * query_cols, axis=-1) / divisor_cols
        gated = (jax.nn.sigmoid(outgate.astype(jnp.float32)) * readout).astype(jnp.bfloat16)
        gated_rows = full_rows(gated)
        update = jnp.dot(
            gated_rows,
            lax.all_gather(w_output[layer], "dp", axis=0, tiled=True),
            preferred_element_type=jnp.float32,
        )
        current = (current.astype(jnp.float32) + update).astype(jnp.bfloat16)
        memories.append(new_state)
        normalisers.append(new_norm)
        maxima.append(new_max)
    return (current, jnp.stack(memories), jnp.stack(normalisers), jnp.stack(maxima))


WIRE = jnp.bfloat16
MESH = pl.DeviceIdType.MESH


def fused_kernel(
    tp, dp,
    tokens, gain_in, w_query, w_key, w_value, w_outgate, w_in, w_fg, bias_in, w_output, mem, norm_in, peak_in,
    mixed, state, norm_out, peak_out,
    wq, wk, wv, wo, wi, wp, gain, bias, norm, peak,
    cur, xg, gs, cg, part, got, gate_part, gate_got, up_part, up_got, nn,
    small_sem, load_sem, xs_sem, xr_sem, gs_sem, gr_sem, ps_sem, pr_sem, us_sem, ur_sem, ns_sem, nr_sem,
):
    t, d = lax.axis_index("tp"), lax.axis_index("dp")
    seqs, feats = tokens.shape
    rows = wq.shape[1]
    qcols, vcols = wq.shape[2], wv.shape[2]
    group = rows // feats
    own_heads = vcols // DV
    features = gain.shape[1]
    heads = peak.shape[2]
    f32, bf16 = jnp.float32, jnp.bfloat16

    smalls = []
    for i, (src, dst) in enumerate(
        ((tokens, cur.at[0]), (gain_in, gain), (bias_in, bias), (norm_in, norm), (peak_in, peak))
    ):
        c = pltpu.make_async_copy(src, dst, small_sem.at[i])
        c.start()
        smalls.append(c)
    loads = {}
    order = ((w_in, wi), (w_fg, wi), (w_query, wq), (w_key, wk), (w_value, wv), (w_outgate, wo), (mem, state), (w_output, wp))
    for b in range(BLOCKS):
        for i, (src, dst) in enumerate(order):
            to = dst.at[b, pl.ds(i * heads, heads)] if i < 2 else dst.at[b]
            c = pltpu.make_async_copy(src.at[b], to, load_sem.at[b, i])
            c.start()
            loads[b, i] = c

    barrier = pltpu.get_barrier_semaphore()
    for i in range(tp):
        for j in range(dp):
            if i + j > 0:
                there = {"tp": (t + i) % tp, "dp": (d + j) % dp}
                pl.semaphore_signal(barrier, inc=1, device_id=there, device_id_type=MESH)
    gate_part[...] = jnp.zeros_like(gate_part)
    for c in smalls:
        c.wait()
    pl.semaphore_wait(barrier, tp * dp - 1)

    sends = []

    def spread(src, dst, send_sem, recv_sem):
        home, slot = t // group, t % group
        here = home == d

        def to(target, k):
            return pltpu.make_async_remote_copy(
                src_ref=src, dst_ref=dst.at[d, slot], send_sem=send_sem.at[k], recv_sem=recv_sem.at[d, slot],
                device_id={"tp": target, "dp": home}, device_id_type=MESH,
            )

        for k in range(tp - 1, 0, -1):
            c = to((t + k) % tp, k)
            c.start()
            sends.append((None, c))

        @pl.when(jnp.logical_not(here))
        def _():
            to(t, 0).start()

        @pl.when(here)
        def _():
            dst[d, slot] = src[...]

        sends.append((jnp.logical_not(here), to(t, 0)))

    def collect(dst, send_sem, recv_sem, dd, g):
        @pl.when(jnp.logical_or(d * group + g != t, d != dd))
        def _():
            pltpu.make_async_remote_copy(
                src_ref=dst.at[dd, g], dst_ref=dst.at[dd, g], send_sem=send_sem.at[0], recv_sem=recv_sem.at[dd, g],
                device_id={"tp": (t + 1) % tp, "dp": d}, device_id_type=MESH,
            ).wait_recv()

    def to_owners(src, dst, send_sem, recv_sem, view):
        copies = []
        for k in range(1, dp):
            dd = (d + k) % dp
            c = pltpu.make_async_remote_copy(
                src_ref=src.at[(dd,) + view], dst_ref=dst.at[(k - 1,) + view],
                send_sem=send_sem.at[k - 1], recv_sem=recv_sem.at[k - 1],
                device_id={"tp": t, "dp": dd}, device_id_type=MESH,
            )
            c.start()
            copies.append(c)
            sends.append((None, c))
        return copies

    def total(src, dst, view, copies):
        acc = src[(d,) + view].astype(f32)
        for k in range(dp - 1):
            copies[k].wait_recv()
            acc = acc + dst[(k,) + view].astype(f32)
        return acc

    norms = []
    lane = lax.broadcasted_iota(jnp.int32, (seqs, heads), 1)
    row = lax.broadcasted_iota(jnp.int32, (seqs, DV), 0)
    everything = (slice(None), slice(None))

    for b in range(BLOCKS):
        here = cur.at[b]
        spread(here, xg.at[b], xs_sem.at[b], xr_sem.at[b])
        for dd in range(dp):
            for g in range(group):
                collect(xg.at[b], xs_sem.at[b], xr_sem.at[b], dd, g)
        pieces = []
        square = jnp.zeros((dp * seqs, 1), f32)
        for g in range(group):
            wide = jnp.concatenate([xg[b, dd, g].astype(f32) for dd in range(dp)], axis=0)
            square = square + jnp.sum(wide * wide, axis=1, keepdims=True)
            at = pl.multiple_of(d * rows + g * feats, feats)
            pieces.append((wide * gain[b : b + 1, pl.ds(at, feats)]).astype(bf16))
        x = jnp.concatenate(pieces, axis=1)

        loads[b, 0].wait()
        loads[b, 1].wait()
        pre = lax.dot_general(x, wi[b], (((1,), (1,)), ((), ())), preferred_element_type=f32)
        for dd in range(dp):
            own = slice(dd * seqs, (dd + 1) * seqs)
            gate_part[b, dd, :, 0 : 2 * heads] = pre[own]
            gate_part[b, dd, :, 2 * heads : 2 * heads + 1] = square[own]
        gate_copies = to_owners(gate_part.at[b], gate_got.at[b], ps_sem.at[b, 0], pr_sem.at[b, 0], everything)

        spans, flights, at = [], [], 0
        for chunk, members in enumerate((((2, wq), (3, wk)), ((4, wv),), ((5, wo),))):
            begin = at
            for i, w in members:
                loads[b, i].wait()
                p = jnp.dot(x, w[b], preferred_element_type=f32).astype(WIRE)
                n = w.shape[2]
                for dd in range(dp):
                    part[b, dd, :, at : at + n] = p[dd * seqs : (dd + 1) * seqs]
                at += n
            view = (slice(None), pl.ds(begin, at - begin))
            spans.append(view)
            flights.append(to_owners(part.at[b], got.at[b], ps_sem.at[b, chunk + 1], pr_sem.at[b, chunk + 1], view))

        gates = total(gate_part.at[b], gate_got.at[b], everything, gate_copies)
        scale = lax.rsqrt(gates[:, 2 * heads : 2 * heads + 1] * (1.0 / features) + EPSILON)
        in_pre = gates[:, :heads] * scale
        forget = gates[:, heads : 2 * heads] * scale + bias[b : b + 1, :]
        log_forget = jnp.minimum(forget, 0.0) - jnp.log1p(jnp.exp(-jnp.abs(forget)))
        moved = log_forget + peak[b]
        new_peak = jnp.maximum(moved, in_pre)
        carried = jnp.exp(moved - new_peak)
        fresh = jnp.exp(in_pre - new_peak)
        peak_out[b] = new_peak

        qk = (total(part.at[b], got.at[b], spans[0], flights[0]) * scale).astype(bf16).astype(f32)
        loads[b, 6].wait()
        stage = []
        for hh in range(own_heads):
            mine = lane == t * own_heads + hh
            c_h = jnp.sum(jnp.where(mine, carried, 0.0), axis=1, keepdims=True)
            f_h = jnp.sum(jnp.where(mine, fresh, 0.0), axis=1, keepdims=True)
            q_h = qk[:, hh * DK : (hh + 1) * DK]
            k_h = qk[:, qcols + hh * DK : qcols + (hh + 1) * DK] * DK ** (-0.5)
            n_h = c_h * norm[b, :, t * own_heads + hh, :] + f_h * k_h
            nn[b, t, hh] = n_h
            div = jnp.maximum(jnp.abs(jnp.sum(n_h * q_h, axis=1, keepdims=True)), 1.0)
            kq = jnp.sum(k_h * q_h, axis=1, keepdims=True)
            q_b = q_h.astype(bf16)
            read = jnp.zeros((seqs, DV), f32)
            for s in range(seqs):
                c = state[b, s, hh * DV : (hh + 1) * DV, :].astype(bf16)
                r = lax.dot_general(q_b, c, (((1,), (1,)), ((), ())), preferred_element_type=f32)
                read = read + jnp.where(row == s, r, 0.0)
            stage.append((c_h, f_h, k_h, div, kq, read))

        v = (total(part.at[b], got.at[b], spans[1], flights[1]) * scale).astype(bf16).astype(f32)
        o = (total(part.at[b], got.at[b], spans[2], flights[2]) * scale).astype(bf16).astype(f32)
        for hh, (c_h, f_h, k_h, div, kq, read) in enumerate(stage):
            cols = slice(hh * DV, (hh + 1) * DV)
            readout = (c_h * read + (f_h * kq) * v[:, cols]) / div
            gs[b, :, cols] = (jax.nn.sigmoid(o[:, cols]) * readout).astype(bf16)
        spread(gs.at[b], cg.at[b], gs_sem.at[b], gr_sem.at[b])

        for k in range(1, tp):
            c = pltpu.make_async_remote_copy(
                src_ref=nn.at[b, t], dst_ref=nn.at[b, t], send_sem=ns_sem.at[b, k - 1], recv_sem=nr_sem.at[b, k - 1],
                device_id={"tp": (t + k) % tp, "dp": d}, device_id_type=MESH,
            )
            c.start()
            sends.append((None, c))
            norms.append((k, b))

        for hh, (c_h, f_h, k_h, div, kq, read) in enumerate(stage):
            cols = slice(hh * DV, (hh + 1) * DV)
            v_t = jnp.transpose(v[:, cols] * f_h)
            for s in range(seqs):
                state[b, s, cols, :] = c_h[s : s + 1] * state[b, s, cols, :] + v_t[:, s : s + 1] * k_h[s : s + 1]
        for dd in range(dp):
            for g in range(group):
                collect(cg.at[b], gs_sem.at[b], gr_sem.at[b], dd, g)
        gated = jnp.concatenate(
            [
                jnp.concatenate([cg[b, dd, g].astype(f32) for dd in range(dp)], axis=0).astype(bf16)
                for g in range(group)
            ],
            axis=1,
        )
        loads[b, 7].wait()
        up = jnp.dot(gated, wp[b], preferred_element_type=f32).astype(WIRE)
        for dd in range(dp):
            up_part[b, dd] = up[dd * seqs : (dd + 1) * seqs]
        flat = (slice(None), slice(None))
        copies = to_owners(up_part.at[b], up_got.at[b], us_sem.at[b], ur_sem.at[b], flat)
        update = total(up_part.at[b], up_got.at[b], flat, copies)
        after = (here[...].astype(f32) + update).astype(bf16)
        if b + 1 < BLOCKS:
            cur[b + 1] = after
        else:
            mixed[...] = after

    for k, b in norms:
        pltpu.make_async_remote_copy(
            src_ref=nn.at[b, t], dst_ref=nn.at[b, (t + tp - k) % tp], send_sem=ns_sem.at[b, k - 1],
            recv_sem=nr_sem.at[b, k - 1], device_id={"tp": (t + k) % tp, "dp": d}, device_id_type=MESH,
        ).wait_recv()
    for b in range(BLOCKS):
        for i in range(tp):
            for hh in range(own_heads):
                norm_out[b, :, i * own_heads + hh, :] = nn[b, i, hh]
    for cond, c in sends:
        if cond is None:
            c.wait_send()
        else:
            pl.when(cond)(c.wait_send)


def write_kernel(*refs):
    count = (len(refs) - 1) // 2
    sem = refs[-1]
    copies = [pltpu.make_async_copy(refs[i], refs[count + i], sem.at[i]) for i in range(count)]
    for c in copies:
        c.start()
    for c in copies:
        c.wait()


def written(*arrays):
    return pl.pallas_call(
        write_kernel,
        out_shape=tuple(jax.ShapeDtypeStruct(a.shape, a.dtype) for a in arrays),
        in_specs=[pl.BlockSpec(memory_space=pltpu.VMEM)] * len(arrays),
        out_specs=(pl.BlockSpec(memory_space=pl.ANY),) * len(arrays),
        scratch_shapes=[pltpu.SemaphoreType.DMA((len(arrays),))],
        compiler_params=pltpu.CompilerParams(vmem_limit_bytes=1024 * 1024),
    )(*(pltpu.with_memory_space_constraint(a, pltpu.VMEM) for a in arrays))


def fused(tp, dp, tokens, gain, w_query, w_key, w_value, w_outgate, w_in, w_fg, bias, w_output, mem, norm, peak):
    seqs, feats = tokens.shape
    rows, vcols = w_value.shape[1:]
    group, own_heads = rows // feats, vcols // DV
    heads = peak.shape[2]
    width = 2 * w_query.shape[2] + 2 * vcols
    vmem = pl.BlockSpec(memory_space=pltpu.VMEM)
    f32, bf16 = jnp.float32, jnp.bfloat16
    dma = pltpu.SemaphoreType.DMA
    w_in, w_fg = jnp.swapaxes(w_in, 1, 2), jnp.swapaxes(w_fg, 1, 2)
    arrays = (tokens, gain, w_query, w_key, w_value, w_outgate, w_in, w_fg, bias, w_output, mem, norm, peak)
    gates = (BLOCKS, 2 * heads, rows)
    big = (w_query.shape, w_key.shape, w_value.shape, w_outgate.shape, gates, w_output.shape)
    lanes = -(-(2 * heads + 1) // 128) * 128
    others = max(dp - 1, 1)
    results = pl.pallas_call(
        functools.partial(fused_kernel, tp, dp),
        out_shape=(
            pltpu.VMEM(tokens.shape, tokens.dtype),
            pltpu.VMEM(mem.shape, mem.dtype),
            pltpu.VMEM(norm.shape, f32),
            pltpu.VMEM(peak.shape, f32),
        ),
        in_specs=[pl.BlockSpec(memory_space=pltpu.HBM)] * len(arrays),
        out_specs=(vmem, vmem, vmem, vmem),
        scratch_shapes=[pltpu.VMEM(shape, bf16) for shape in big]
        + [pltpu.VMEM(a.shape, a.dtype) for a in (gain, bias, norm, peak)]
        + [
            pltpu.VMEM((BLOCKS, seqs, feats), bf16),
            pltpu.VMEM((BLOCKS, dp, group, seqs, feats), bf16),
            pltpu.VMEM((BLOCKS, seqs, vcols), bf16),
            pltpu.VMEM((BLOCKS, dp, group, seqs, vcols), bf16),
            pltpu.VMEM((BLOCKS, dp, seqs, width), WIRE),
            pltpu.VMEM((BLOCKS, others, seqs, width), WIRE),
            pltpu.VMEM((BLOCKS, dp, seqs, lanes), f32),
            pltpu.VMEM((BLOCKS, others, seqs, lanes), f32),
            pltpu.VMEM((BLOCKS, dp, seqs, feats), WIRE),
            pltpu.VMEM((BLOCKS, others, seqs, feats), WIRE),
            pltpu.VMEM((BLOCKS, tp, own_heads, seqs, DK), f32),
            dma((5,)),
            dma((BLOCKS, 8)),
            dma((BLOCKS, tp)),
            dma((BLOCKS, dp, group)),
            dma((BLOCKS, tp)),
            dma((BLOCKS, dp, group)),
            dma((BLOCKS, 4, others)),
            dma((BLOCKS, 4, others)),
            dma((BLOCKS, others)),
            dma((BLOCKS, others)),
            dma((BLOCKS, tp)),
            dma((BLOCKS, tp)),
        ],
        compiler_params=pltpu.CompilerParams(
            collective_id=0, has_side_effects=True, vmem_limit_bytes=24 * 1024 * 1024
        ),
    )(*(pltpu.with_memory_space_constraint(a, pltpu.HBM) for a in arrays))
    return written(*results)


def whole_heads(tp, dp, *args):
    tokens, w_query, w_value, w_output = args[0], args[2], args[4], args[9]
    seqs, feats = tokens.shape
    rows, vcols = w_value.shape[1:]
    return (
        tp > 1 and dp > 1 and seqs % 8 == 0 and feats % 128 == 0
        and vcols % DV == 0 and w_query.shape[2] == vcols // DV * DK
        and rows % feats == 0 and vcols == feats and w_output.shape[1] == rows
    )


def shards(tp, dp, *args):
    if whole_heads(tp, dp, *args):
        return fused(tp, dp, *args)
    return gathered(*args)


def solution(mesh):
    in_specs = (
        P("dp", "tp"),
        P(),
        P(None, "dp", "tp"),
        P(None, "dp", "tp"),
        P(None, "dp", "tp"),
        P(None, "dp", "tp"),
        P(None, "dp", None),
        P(None, "dp", None),
        P(),
        P(None, "dp", "tp"),
        P(None, "dp", "tp", None),
        P(None, "dp", None, None),
        P(None, "dp", None),
    )
    out_specs = (
        P("dp", "tp"),
        P(None, "dp", "tp", None),
        P(None, "dp", None, None),
        P(None, "dp", None),
    )
    body = functools.partial(shards, mesh.shape["tp"], mesh.shape["dp"])
    return jax.shard_map(body, mesh=mesh, in_specs=in_specs, out_specs=out_specs, check_vma=False)
```
